32 devices in a mesh: grp: 2 (over x), ep: 4 (over y, core), tp: 4 (over z).
Axes of the slice: x: 2, y: 2, z: 4, core: 2. Of those that a mesh axis runs over, the one named last changes fastest.
Arguments:
- pool_input: bfloat16 [8192, 1024], P(('grp', 'ep'), 'tp'), parts along dimension 0, may hold values from -6 to 6
- pool_map: bfloat16 [8, 128, 128], replicated, may hold values from -0.5 to 0.5
- pool_scale: float32 [1024], replicated, may hold values from 0.1 to 1.9
- out_weight: bfloat16 [1024, 2048], P(None, 'tp'), may hold values from -0.1875 to 0.1875
- expert_input: bfloat16 [4096, 2048], P(('grp', 'ep', 'tp')), parts along dimension 0, may hold values from -6 to 6
- norm_gain: float32 [2048], replicated, may hold values from 0.1 to 1.9
- routes: int32 [4096, 2], P(('grp', 'ep', 'tp')), parts along dimension 0, may hold values from 0 to 15, all different within a row; in each aligned block of 128 rows (0 to 127, 128 to 255, ...) at most 32 rows name the same one
- route_weight: float32 [4096, 2], P(('grp', 'ep', 'tp')), parts along dimension 0, may hold values from 0.2 to 1.5
- gate_weight: bfloat16 [16, 2048, 512], P(('ep', 'tp')), may hold values from -0.125 to 0.125
- up_weight: bfloat16 [16, 2048, 512], P(('ep', 'tp')), may hold values from -0.125 to 0.125
- down_weight: bfloat16 [16, 512, 2048], P(('ep', 'tp')), may hold values from -0.25 to 0.25
Outputs:
- pool_output: bfloat16 [8192, 2048], P(('grp', 'ep'), 'tp'), parts along dimension 0
- expert_output: bfloat16 [4096, 2048], P(('grp', 'ep', 'tp')), parts along dimension 0
The draws below stay inside these ranges and needn't reach their ends.
There are 2 independent parts, one for each index of `grp`. The reference program is written for one: setup_inputs(seed, part) draws one part's arguments, and reference() takes and returns one part's arrays. A program takes and returns all parts, laid end to end along the dimension named above; an argument that names none is the same for every part. Nothing has to cross between parts.
Inputs may be any that keep to these rules, and one draw needn't show every extreme that they name: `routes`: each row names 2 different experts. In the rows of one device no expert is named more than 32 times, and in every draw some device names some expert exactly 32 times.
All inputs are finite; a program needn't handle non-finite values.
Results may differ from the reference program's by a relative error of at most 0.007.
Values may be sent and summed in bfloat16 or wider, within the bound.
A program may use at most 64 MiB of HBM per device.

```python
import math
import jax
import jax.numpy as jnp
import numpy as np
from jax import lax

D = 2048
D_EXPERT = 512
GROUP_DIM = 128
GROUPS = 8
TOP_K = 2
ROWS_B = 128
D_POOL = 1024
EXPERTS = 16
CAP = 32
TOKENS_A = 4096
TOKENS_B = 2048
N_EP = 4
N_TP = 4


def shard_levels(key, shape, split, low, top_value):
    loudness = 1.0
    for position, blocks in split:
        draws = jax.random.uniform(jax.random.fold_in(jax.random.fold_in(key, 6), position), (blocks,), jnp.float32, low / len(split), top_value / len(split))
        loudness = loudness * jnp.repeat(jnp.exp(draws), shape[position] // blocks).reshape((-1,) + (1,) * (len(shape) - 1 - position))
    return loudness


def routed_block(key, own, number, rows, amount, top, bound, skew):
    sequence = jax.random.permutation(key, amount)
    heavy_load, common = shares(amount, rows * top, bound, skew, True), shares(amount, rows * top, bound, skew, False)
    places = jnp.arange(amount)

    def named(tallies, turn):
        used = int((tallies > 0).sum())
        fixed = max(1, used // 4)
        moved = fixed + (places - fixed + turn * (used - fixed)) % max(1, amount - fixed)
        return jnp.zeros((amount,), jnp.int32).at[sequence[jnp.where(places < fixed, places, moved)]].set(jnp.asarray(tallies, jnp.int32))

    tallies = jnp.where(number % 4 == 0, named(heavy_load, number // 4), named(common, number - number // 4 - 1))
    mixed = jax.random.permutation(jax.random.fold_in(own, 3), amount)
    giver, receiver = mixed[0:amount // 2 * 2:2], mixed[1:amount // 2 * 2:2]
    margin = jnp.minimum(tallies[giver] - 1, bound - tallies[receiver]) // 2
    margin = jnp.where((giver == sequence[0]) | (receiver == sequence[0]) | (tallies[receiver] == 0), 0, jnp.maximum(margin, 0))
    moved = jax.random.randint(jax.random.fold_in(own, 4), (amount // 2,), 0, 1 << 20) % (margin + 1)
    tallies = tallies.at[giver].add(-moved).at[receiver].add(moved)
    labels = jnp.searchsorted(jnp.cumsum(tallies), jnp.arange(rows * top), side="right").astype(jnp.int32)
    grid = labels.reshape(top, rows).T
    grid = grid[jax.random.permutation(jax.random.fold_in(own, 1), rows)]
    turn = jax.random.randint(jax.random.fold_in(own, 2), (rows, 1), 0, top)
    return jnp.take_along_axis(grid, (jnp.arange(top)[None, :] + turn) % top, axis=1)


def shares(amount, total, limit, skew, full):
    weights = [(1 << 20) // math.isqrt(standing ** skew) + 1 for standing in range(1, amount + 1)]
    largest = limit if full else min(limit, max(-(-total // amount), total * weights[0] // sum(weights)))
    least = 1 if total - largest >= amount - 1 else 0
    given, spare = [largest] + [least] * (amount - 1), total - largest - least * (amount - 1)
    while spare > 0:
        candidates = [i for i in range(1, amount) if given[i] < largest] or [i for i in range(1, amount) if given[i] < limit]
        whole, remaining = sum([weights[i] for i in candidates]), spare
        for i in candidates:
            more = min(limit - given[i], max(1, remaining * weights[i] // whole), spare)
            given[i] = given[i] + more
            spare = spare - more
    return np.array(given)


def scatter_about(stream_key, shape, width, bound, pieces=(), held_as=jnp.bfloat16):
    values = jax.random.normal(stream_key, shape, jnp.float32) * width
    if len(pieces) > 0:
        values = shard_levels(stream_key, shape, pieces, -0.22, 0.18) * values
    return jnp.clip(values, min=-bound, max=bound).astype(held_as)


def setup_inputs(seed: int = 0, part: int = 0) -> dict:
    seeds = jax.random.split(jax.random.key(seed), 12)
    part_splits = jax.random.split(jax.random.fold_in(seeds[11], part), 12)
    pool_input = scatter_about(part_splits[0], (TOKENS_A, D_POOL), 1.0, 6.0, ((0, 4), (1, 4)))
    pool_map = scatter_about(seeds[1], (GROUPS, GROUP_DIM, GROUP_DIM), GROUP_DIM ** -0.5, 0.5)
    pool_scale = jnp.clip(1.0 + 0.18 * jax.random.normal(seeds[2], (D_POOL,), jnp.float32), 0.1, 1.9)
    out_weight = scatter_about(seeds[3], (D_POOL, D), D_POOL ** -0.5, 0.1875, ((1, 4),))
    expert_input = scatter_about(part_splits[4], (TOKENS_B, D), 1.0, 6.0, ((0, 16),))
    norm_gain = jnp.clip(1.0 + 0.18 * jax.random.normal(seeds[5], (D,), jnp.float32), 0.1, 1.9)
    routes_keys = jax.random.split(jax.random.fold_in(part_splits[6], 1), TOKENS_B // ROWS_B)
    routes_turns = jax.random.permutation(jax.random.fold_in(part_splits[6], 3), TOKENS_B // ROWS_B)
    routes = jax.vmap(lambda own, number: routed_block(jax.random.fold_in(part_splits[6], 2), own, number, ROWS_B, EXPERTS, TOP_K, CAP, 2))(routes_keys, routes_turns).reshape((TOKENS_B, TOP_K))
    route_weight = jnp.clip(0.2 + 1.3 * jax.random.uniform(part_splits[7], (TOKENS_B, TOP_K), jnp.float32) ** shard_levels(part_splits[7], (TOKENS_B, TOP_K), ((0, 16),), -0.2, 0.2), 0.2, 1.5)
    gate_weight = scatter_about(seeds[8], (EXPERTS, D, D_EXPERT), D ** -0.5, 0.125, ((0, 16),))
    up_weight = scatter_about(seeds[9], (EXPERTS, D, D_EXPERT), D ** -0.5, 0.125, ((0, 16),))
    down_weight = scatter_about(seeds[10], (EXPERTS, D_EXPERT, D), D_EXPERT ** -0.5, 0.25, ((0, 16),))
    return {"pool_input": pool_input, "pool_map": pool_map, "pool_scale": pool_scale, "out_weight": out_weight, "expert_input": expert_input, "norm_gain": norm_gain, "routes": routes, "route_weight": route_weight, "gate_weight": gate_weight, "up_weight": up_weight, "down_weight": down_weight}


epsilon = 1e-06

def pool_group(column_block, window):
    length = column_block.shape[0]
    running = jnp.cumsum(column_block, axis=0)
    earlier = jnp.pad(running, ((window, 0), (0, 0)))[:length]
    counted = jnp.minimum(jnp.arange(length) + 1, window).astype(jnp.float32)
    return (running - earlier) / counted[:, None] - column_block

def reference(pool_input, pool_map, pool_scale, out_weight, expert_input, norm_gain, routes, route_weight, gate_weight, up_weight, down_weight):
    widened = pool_input.astype(jnp.float32)
    mapped_parts = []
    for group_index in range(GROUPS):
        window = 2 ** (1 + group_index % 4)
        lower = group_index * GROUP_DIM
        columns = widened[:, lower:lower + GROUP_DIM]
        pooled = pool_group(columns, window).astype(jnp.bfloat16)
        mapped = jnp.dot(pooled, pool_map[group_index], preferred_element_type=jnp.float32)
        mapped = mapped * pool_scale[lower:lower + GROUP_DIM]
        mapped_parts.append(mapped.astype(jnp.bfloat16))
    mapped_all = jnp.concatenate(mapped_parts, axis=1)
    pool_output = jnp.dot(mapped_all, out_weight, preferred_element_type=jnp.float32).astype(jnp.bfloat16)
    widened_b = expert_input.astype(jnp.float32)
    normed = widened_b * lax.rsqrt(lax.optimization_barrier(jnp.mean(widened_b * widened_b, axis=1, keepdims=True)) + epsilon) * norm_gain
    normed = normed.astype(jnp.bfloat16)
    devices_all = N_EP * N_TP
    copies = ROWS_B * TOP_K
    flat_routes = routes.reshape(devices_all, copies).astype(jnp.int32)
    onehot = (flat_routes[:, :, None] == jnp.arange(EXPERTS, dtype=jnp.int32)[None, None, :]).astype(jnp.int32)
    before = jnp.cumsum(onehot, axis=1) - onehot
    slot_index = lax.optimization_barrier(jnp.sum(before * onehot, axis=2)).astype(jnp.int32)
    device_of = jnp.arange(devices_all, dtype=jnp.int32)[:, None]
    target = (flat_routes * (devices_all * CAP) + device_of * CAP + slot_index).astype(jnp.int32)
    token_of = (device_of * ROWS_B + jnp.arange(copies, dtype=jnp.int32)[None, :] // TOP_K).astype(jnp.int32)
    slot_count = EXPERTS * devices_all * CAP
    slot_table = jnp.full((slot_count,), TOKENS_B, jnp.int32).at[target.reshape(-1)].set(token_of.reshape(-1))
    slot_weight = jnp.zeros((slot_count,), jnp.float32).at[target.reshape(-1)].set(route_weight.astype(jnp.float32).reshape(-1))
    padded = jnp.concatenate([normed, jnp.zeros((1, D), jnp.bfloat16)], axis=0)

    def one_expert(accumulated, inputs):
        tokens_here, weights_here, gate_here, up_here, down_here = inputs
        rows_here = padded[tokens_here]
        gate_part = jnp.dot(rows_here, gate_here, preferred_element_type=jnp.float32)
        up_part = jnp.dot(rows_here, up_here, preferred_element_type=jnp.float32)
        hidden = (jax.nn.silu(gate_part) * up_part).astype(jnp.bfloat16)
        result = jnp.dot(hidden, down_here, preferred_element_type=jnp.float32).astype(jnp.bfloat16)
        accumulated = accumulated.at[tokens_here].add(weights_here[:, None] * result.astype(jnp.float32))
        return (accumulated, None)
    initial = jnp.zeros((TOKENS_B + 1, D), jnp.float32)
    accumulated, unused = lax.scan(one_expert, initial, (slot_table.reshape(EXPERTS, -1), slot_weight.reshape(EXPERTS, -1), gate_weight, up_weight, down_weight))
    expert_output = accumulated[:TOKENS_B].astype(jnp.bfloat16)
    return (pool_output, expert_output)
```

```python
import functools

import jax
import jax.numpy as jnp
from jax import lax
from jax.experimental import pallas as pl
from jax.experimental.pallas import tpu as pltpu
from jax.sharding import PartitionSpec as P

epsilon = 1e-06
halo_depth = 16
MESH = pl.DeviceIdType.MESH
bf16 = jnp.bfloat16
f32 = jnp.float32


def shifted_2(shard, axis, by):
    size = lax.axis_size(axis)
    pairs = [(i, i + by) for i in range(size) if 0 <= i + by < size]
    return lax.ppermute(shard, axis, pairs)


def mapped_channels(pool_input, pool_map, pool_scale):
    row_count, width_local = pool_input.shape
    group_dim = pool_map.shape[1]
    groups_local = width_local // group_dim
    last_rows = pool_input[row_count - halo_depth :]
    earlier_rows = shifted_2(last_rows, "ep", 1)
    extended = jnp.concatenate([earlier_rows, pool_input], axis=0).astype(f32)
    first_group = lax.axis_index("tp") * groups_local
    group_ids = first_group + jnp.arange(width_local, dtype=jnp.int32) // group_dim
    window = jnp.left_shift(jnp.int32(2), group_ids % 4)
    summed = jnp.zeros((row_count, width_local), f32)
    for offset in range(halo_depth):
        shifted = extended[halo_depth - offset : halo_depth - offset + row_count]
        summed = summed + jnp.where(offset < window, shifted, 0.0)
    positions = lax.axis_index("ep") * row_count + jnp.arange(row_count, dtype=jnp.int32)
    counted = jnp.minimum(positions[:, None] + 1, window[None, :]).astype(f32)
    pooled = (summed / counted - extended[halo_depth:]).astype(bf16)
    maps_local = lax.dynamic_slice_in_dim(pool_map, first_group, groups_local, 0)
    scales_local = lax.dynamic_slice_in_dim(pool_scale, first_group * group_dim, width_local, 0)
    mapped = jnp.einsum(
        "rgc,gcd->rgd",
        pooled.reshape(row_count, groups_local, group_dim),
        maps_local,
        preferred_element_type=f32,
    )
    return (mapped.reshape(row_count, width_local) * scales_local).astype(bf16)


def route_codes(routes, route_weight, n_ep, n_tp, capacity):
    row_count, top = routes.shape
    experts = n_ep * n_tp
    flat = routes.reshape(row_count * top)
    onehot = (flat[:, None] == jnp.arange(experts, dtype=jnp.int32)[None, :]).astype(f32)
    copies = row_count * top
    earlier = (
        jnp.arange(copies, dtype=jnp.int32)[:, None] > jnp.arange(copies, dtype=jnp.int32)[None, :]
    ).astype(f32)
    before = jnp.dot(earlier, onehot, preferred_element_type=f32)
    slot = jnp.sum(before * onehot, axis=1).astype(jnp.int32)
    code = (flat % n_tp) * (n_ep * capacity) + (flat // n_tp) * capacity + slot
    codes = code.reshape(row_count, top).T.astype(f32)
    meta = jnp.concatenate([codes, route_weight.T.astype(f32)], axis=0)
    return jnp.pad(meta, ((0, -meta.shape[0] % 8), (0, 0)))


def kernel(
    n, n_ep, cap, top,
    x_ref, meta_ref, pool_ref, gate_hbm, up_hbm, down_hbm, out_w_hbm,
    pool_out, expert_out,
    wg, wu, wd, wo, tok, meta, pools, packed, rows, back, hidden, part, from_left, from_right, acc,
    w_sem, tok_recv, tok_right, tok_left, meta_recv, meta_right, meta_left,
    pool_recv, pool_right, pool_left, pk_send, pk_recv, bk_send, bk_recv,
    rs_right, rs_right_recv, rs_left, rs_left_recv,
):
    me = lax.axis_index("tp")
    mine = lax.axis_index("ep")
    slots = n_ep * cap
    width = x_ref.shape[1]
    d_expert = wg.shape[1]
    shard = pool_ref.shape[1]
    has_left, has_right = me > 0, me < n - 1

    def peer(q):
        return lax.rem(mine + q, n_ep)

    def at_slots(p):
        return pl.ds(pl.multiple_of(p * cap, cap), cap)

    loads = [
        pltpu.make_async_copy(src, dst, w_sem.at[i])
        for i, (src, dst) in enumerate(
            ((gate_hbm.at[0], wg), (up_hbm.at[0], wu), (down_hbm.at[0], wd), (out_w_hbm, wo))
        )
    ]
    for load in loads:
        load.start()

    barrier = pltpu.get_barrier_semaphore()

    @pl.when(has_left)
    def _():
        pl.semaphore_signal(barrier, inc=1, device_id={"tp": me - 1}, device_id_type=MESH)

    @pl.when(has_right)
    def _():
        pl.semaphore_signal(barrier, inc=1, device_id={"tp": me + 1}, device_id_type=MESH)

    for q in range(1, n_ep):
        pl.semaphore_signal(barrier, inc=1, device_id={"ep": peer(q)}, device_id_type=MESH)
    neighbours = jnp.where(has_left, 1, 0) + jnp.where(has_right, 1, 0)
    pl.semaphore_wait(barrier, n_ep - 1 + neighbours)

    def source(j):
        least = jnp.minimum(me, n - 1 - me)
        k = (j + 1) // 2
        near = jnp.where(j % 2 == 1, me - k, me + k)
        k_far = j - least
        far = jnp.where(me > n - 1 - me, me - k_far, me + k_far)
        return jnp.where(j <= 2 * least, near, far)

    def hop(src, buffer, s, send, recv, step):
        return pltpu.make_async_remote_copy(
            src_ref=src, dst_ref=buffer.at[s], send_sem=send.at[s], recv_sem=recv.at[s],
            device_id={"tp": me + step}, device_id_type=MESH,
        )

    token_lane = ((tok, tok_right, tok_left, tok_recv), (meta, meta_right, meta_left, meta_recv))
    pool_lane = ((pools, pool_right, pool_left, pool_recv),)

    def pass_on(lane, s, own):
        @pl.when((s <= me) & has_right)
        def _():
            for i, (buffer, right, left, recv) in enumerate(lane):
                hop(own[i] if own else buffer.at[s], buffer, s, right, recv, 1).start()

        @pl.when((s >= me) & has_left)
        def _():
            for i, (buffer, right, left, recv) in enumerate(lane):
                hop(own[i] if own else buffer.at[s], buffer, s, left, recv, -1).start()

    def arrive(lane, s):
        for buffer, right, left, recv in lane:
            hop(buffer.at[s], buffer, s, right, recv, 1).wait_recv()

    def passed(lane, s, own):
        @pl.when((s <= me) & has_right)
        def _():
            for buffer, right, left, recv in lane:
                hop(buffer.at[s], buffer, s, right, recv, 1).wait_send()

        @pl.when((s >= me) & has_left)
        def _():
            for buffer, right, left, recv in lane:
                hop(buffer.at[s], buffer, s, left, recv, -1).wait_send()

    def exchange(src, dst, s, p, send, recv):
        return pltpu.make_async_remote_copy(
            src_ref=src.at[s, at_slots(p)], dst_ref=dst.at[s, at_slots(mine)],
            send_sem=send.at[s, p], recv_sem=recv.at[s, mine],
            device_id={"ep": p}, device_id_type=MESH,
        )

    def exchanged(dst, s, p, send, recv):
        return pltpu.make_async_remote_copy(
            src_ref=dst.at[s, at_slots(p)], dst_ref=dst.at[s, at_slots(p)],
            send_sem=send.at[s, p], recv_sem=recv.at[s, p],
            device_id={"ep": p}, device_id_type=MESH,
        )

    def tiles(total, size):
        return total // size, lambda i: pl.ds(pl.multiple_of(i * size, size), size)

    def slot_masks(s, use_weight):
        row = lax.broadcasted_iota(jnp.int32, (slots, x_ref.shape[0]), 0) + me * slots
        row = row.astype(f32)
        held = meta[s]
        total = jnp.zeros((slots, x_ref.shape[0]), f32)
        for k in range(top):
            value = held[top + k : top + k + 1] if use_weight else 1.0
            total = total + jnp.where(row == held[k : k + 1], value, 0.0)
        return total

    tile_w = min(512, width)
    count_w, at_w = tiles(width, tile_w)
    tile_h = min(256, d_expert)
    count_h, at_h = tiles(d_expert, tile_h)
    tile_r = min(256, pool_ref.shape[0])
    count_r, at_r = tiles(pool_ref.shape[0], tile_r)

    def pack(s):
        choose = slot_masks(s, False).astype(bf16)

        def tile(i, _):
            packed[s, :, at_w(i)] = jnp.dot(
                choose, tok[s, :, at_w(i)], preferred_element_type=f32
            ).astype(bf16)
            return 0

        lax.fori_loop(0, count_w, tile, 0)
        for q in range(1, n_ep):
            exchange(packed, rows, s, peer(q), pk_send, pk_recv).start()
        rows[s, at_slots(mine)] = packed[s, at_slots(mine)]

    def expert(s):
        for q in range(1, n_ep):
            exchanged(rows, s, peer(q), pk_send, pk_recv).wait_recv()

        def inner(i, _):
            here = rows[s]
            gate = jnp.dot(here, wg[:, at_h(i)], preferred_element_type=f32)
            up = jnp.dot(here, wu[:, at_h(i)], preferred_element_type=f32)
            hidden[:, at_h(i)] = (gate / (1.0 + jnp.exp(-gate)) * up).astype(bf16)
            return 0

        lax.fori_loop(0, count_h, inner, 0)

        def outer(i, _):
            rows[s, :, at_w(i)] = jnp.dot(
                hidden[...], wd[:, at_w(i)], preferred_element_type=f32
            ).astype(bf16)
            return 0

        lax.fori_loop(0, count_w, outer, 0)
        for q in range(1, n_ep):
            exchange(rows, back, s, peer(q), bk_send, bk_recv).start()
        back[s, at_slots(mine)] = rows[s, at_slots(mine)]

    def rs_hop(src, buffer, d, send, recv, step):
        return pltpu.make_async_remote_copy(
            src_ref=src.at[d], dst_ref=buffer.at[d], send_sem=send.at[d], recv_sem=recv.at[d],
            device_id={"tp": me + step}, device_id_type=MESH,
        )

    def combine(s):
        for q in range(1, n_ep):
            exchanged(back, s, peer(q), bk_send, bk_recv).wait_recv()
        weights = slot_masks(s, True)
        high = weights.astype(bf16)
        low = (weights - high.astype(f32)).astype(bf16)
        dims = (((0,), (0,)), ((), ()))

        def tile(i, _):
            here = back[s, :, at_w(i)]
            part[s, :, at_w(i)] = (
                lax.dot_general(high, here, dims, preferred_element_type=f32)
                + lax.dot_general(low, here, dims, preferred_element_type=f32)
            ).astype(bf16)
            return 0

        lax.fori_loop(0, count_w, tile, 0)

        @pl.when((me == 0) & (s > me))
        def _():
            rs_hop(part, from_left, s, rs_right, rs_right_recv, 1).start()

        @pl.when((me == n - 1) & (s < me))
        def _():
            rs_hop(part, from_right, s, rs_left, rs_left_recv, -1).start()

    def project(s, first):
        def tile(i, _):
            lhs = pool_ref[at_r(i), :] if first else pools[s, at_r(i), :]
            product = jnp.dot(
                lhs, wo[pl.ds(pl.multiple_of(s * shard, shard), shard), :],
                preferred_element_type=f32,
            )
            acc[at_r(i), :] = product if first else acc[at_r(i), :] + product
            return 0

        lax.fori_loop(0, count_r, tile, 0)

    def add_into(buffer, d):
        def tile(i, _):
            buffer[d, :, at_w(i)] = (
                buffer[d, :, at_w(i)].astype(f32) + part[d, :, at_w(i)].astype(f32)
            ).astype(bf16)
            return 0

        lax.fori_loop(0, count_w, tile, 0)

    pass_on(token_lane, me, (x_ref, meta_ref))

    def own(i, _):
        tok[me, :, at_w(i)] = x_ref[:, at_w(i)]
        return 0

    lax.fori_loop(0, count_w, own, 0)
    meta[me] = meta_ref[...]
    loads[3].wait()
    project(me, True)

    def step(j, _):
        @pl.when(j < n)
        def _():
            s = source(j)

            @pl.when(j > 0)
            def _():
                arrive(token_lane, s)
                pass_on(token_lane, s, None)

            @pl.when((s == 0) & has_right)
            def _():
                hop(pool_ref, pools, me, pool_right, pool_recv, 1).start()

            @pl.when((s == n - 1) & has_left)
            def _():
                hop(pool_ref, pools, me, pool_left, pool_recv, -1).start()

            pack(s)

        @pl.when(j == 1)
        def _():
            for load in loads[:3]:
                load.wait()

        @pl.when((j >= 1) & (j <= n))
        def _():
            expert(source(j - 1))

        @pl.when(j >= 2)
        def _():
            combine(source(j - 2))

        return 0

    lax.fori_loop(0, n + 2, step, 0)

    def tail(i, _):
        s = source(i + 1)
        arrive(pool_lane, s)
        pass_on(pool_lane, s, None)
        project(s, False)
        right, left = i + 1, n - 2 - i

        @pl.when((me > 0) & (me < right))
        def _():
            rs_hop(part, from_left, right, rs_right, rs_right_recv, 1).wait_recv()
            add_into(from_left, right)
            rs_hop(from_left, from_left, right, rs_right, rs_right_recv, 1).start()

        @pl.when((me < n - 1) & (me > left))
        def _():
            rs_hop(part, from_right, left, rs_left, rs_left_recv, -1).wait_recv()
            add_into(from_right, left)
            rs_hop(from_right, from_right, left, rs_left, rs_left_recv, -1).start()

        return 0

    lax.fori_loop(0, n - 1, tail, 0)
    pool_out[...] = acc[...].astype(bf16)
    expert_total = part[me].astype(f32)
    acc_rows = expert_out

    @pl.when(has_left)
    def _():
        rs_hop(part, from_left, me, rs_right, rs_right_recv, 1).wait_recv()

    @pl.when(has_right)
    def _():
        rs_hop(part, from_right, me, rs_left, rs_left_recv, -1).wait_recv()

    @pl.when(has_left & has_right)
    def _():
        acc_rows[...] = (
            expert_total + from_left[me].astype(f32) + from_right[me].astype(f32)
        ).astype(bf16)

    @pl.when(has_left & jnp.logical_not(has_right))
    def _():
        acc_rows[...] = (expert_total + from_left[me].astype(f32)).astype(bf16)

    @pl.when(has_right & jnp.logical_not(has_left))
    def _():
        acc_rows[...] = (expert_total + from_right[me].astype(f32)).astype(bf16)

    def drain(s, _):
        passed(token_lane, s, None)
        passed(pool_lane, s, None)
        for q in range(1, n_ep):
            exchange(packed, rows, s, peer(q), pk_send, pk_recv).wait_send()
            exchange(rows, back, s, peer(q), bk_send, bk_recv).wait_send()

        @pl.when(me < s)
        def _():
            rs_hop(part, from_left, s, rs_right, rs_right_recv, 1).wait_send()

        @pl.when(me > s)
        def _():
            rs_hop(part, from_right, s, rs_left, rs_left_recv, -1).wait_send()

        return 0

    lax.fori_loop(0, n, drain, 0)


def on_device(
    pool_input, pool_map, pool_scale, out_weight, expert_input, norm_gain,
    routes, route_weight, gate_weight, up_weight, down_weight,
):
    n_ep, n = lax.axis_size("ep"), lax.axis_size("tp")
    tokens, width = expert_input.shape
    top = routes.shape[1]
    cap = max(2 * tokens * top // (n_ep * n), 16)
    slots = n_ep * cap
    widened = expert_input.astype(f32)
    normed = widened * lax.rsqrt(jnp.mean(widened * widened, axis=1, keepdims=True) + epsilon)
    normed = (normed * norm_gain).astype(bf16)
    meta = route_codes(routes, route_weight, n_ep, n, cap)
    mapped = mapped_channels(pool_input, pool_map, pool_scale)
    d_expert = gate_weight.shape[2]
    dma = pltpu.SemaphoreType.DMA
    vmem = pl.BlockSpec(memory_space=pltpu.VMEM)
    hbm = pl.BlockSpec(memory_space=pl.ANY)
    line = dma((n,))
    pair = dma((n, n_ep))
    return pl.pallas_call(
        functools.partial(kernel, n, n_ep, cap, top),
        out_shape=(
            jax.ShapeDtypeStruct((mapped.shape[0], out_weight.shape[1]), bf16),
            jax.ShapeDtypeStruct((tokens, width), bf16),
        ),
        in_specs=[vmem] * 3 + [hbm] * 4,
        out_specs=(vmem, vmem),
        scratch_shapes=[
            pltpu.VMEM((width, d_expert), bf16),
            pltpu.VMEM((width, d_expert), bf16),
            pltpu.VMEM((d_expert, width), bf16),
            pltpu.VMEM(out_weight.shape, bf16),
            pltpu.VMEM((n, tokens, width), bf16),
            pltpu.VMEM((n,) + meta.shape, f32),
            pltpu.VMEM((n,) + mapped.shape, bf16),
            pltpu.VMEM((n, slots, width), bf16),
            pltpu.VMEM((n, slots, width), bf16),
            pltpu.VMEM((n, slots, width), bf16),
            pltpu.VMEM((slots, d_expert), bf16),
            pltpu.VMEM((n, tokens, width), bf16),
            pltpu.VMEM((n, tokens, width), bf16),
            pltpu.VMEM((n, tokens, width), bf16),
            pltpu.VMEM((mapped.shape[0], out_weight.shape[1]), f32),
            dma((4,)),
            line, line, line, line, line, line, line, line, line,
            pair, pair, pair, pair,
            line, line, line, line,
        ],
        compiler_params=pltpu.CompilerParams(
            collective_id=0, has_side_effects=True, vmem_limit_bytes=62 * 1024 * 1024
        ),
    )(normed, meta, mapped, gate_weight, up_weight, down_weight, out_weight)


def solution(mesh):
    return jax.shard_map(
        on_device,
        mesh=mesh,
        in_specs=(
            P(("grp", "ep"), "tp"),
            P(),
            P(),
            P(None, "tp"),
            P(("grp", "ep", "tp"), None),
            P(),
            P(("grp", "ep", "tp"), None),
            P(("grp", "ep", "tp"), None),
            P(("ep", "tp"), None, None),
            P(("ep", "tp"), None, None),
            P(("ep", "tp"), None, None),
        ),
        out_specs=(P(("grp", "ep"), "tp"), P(("grp", "ep", "tp"), None)),
        check_vma=False,
    )
```

```python
import functools

import jax
import jax.numpy as jnp
from jax import lax
from jax.experimental import pallas as pl
from jax.experimental.pallas import tpu as pltpu
from jax.sharding import PartitionSpec as P

epsilon = 1e-06
halo_depth = 16
MESH = pl.DeviceIdType.MESH
bf16 = jnp.bfloat16
f32 = jnp.float32


def kernel(
    n, n_ep, cap, top, chunks,
    x_ref, gain_ref, routes_ref, pool_ref, map_ref, scale_ref, gate_hbm, up_hbm, down_hbm, out_w_hbm,
    pool_out, expert_out,
    wg, wu, wd, wo, tok, meta, pools, packed, rows, back, gates, ups, hidden,
    part, from_left, from_right, acc, halo, extended,
    w_sem, halo_send, halo_recv, tok_recv, tok_right, tok_left, meta_recv, meta_right, meta_left,
    pool_recv, pool_right, pool_left, pk_send, pk_recv, bk_send, bk_recv,
    rs_right, rs_right_recv, rs_left, rs_left_recv,
):
    me = lax.axis_index("tp")
    mine = lax.axis_index("ep")
    tokens, width = x_ref.shape
    slots = n_ep * cap
    d_expert = wg.shape[1]
    row_count, shard = pool_ref.shape
    group_dim = map_ref.shape[1]
    groups_local = shard // group_dim
    wc = width // chunks
    has_left, has_right = me > 0, me < n - 1

    def peer(q):
        return lax.rem(mine + q, n_ep)

    def at_slots(p):
        return pl.ds(pl.multiple_of(p * cap, cap), cap)

    def at_chunk(c):
        return pl.ds(pl.multiple_of(c * wc, wc), wc)

    def each(count, body):
        def run(i, _):
            body(i)
            return 0

        lax.fori_loop(0, count, run, 0)

    loads = [
        pltpu.make_async_copy(src, dst, w_sem.at[i])
        for i, (src, dst) in enumerate(
            ((gate_hbm.at[0], wg), (up_hbm.at[0], wu), (down_hbm.at[0], wd), (out_w_hbm, wo))
        )
    ]
    for load in loads:
        load.start()

    barrier = pltpu.get_barrier_semaphore()

    @pl.when(has_left)
    def _():
        pl.semaphore_signal(barrier, inc=1, device_id={"tp": me - 1}, device_id_type=MESH)

    @pl.when(has_right)
    def _():
        pl.semaphore_signal(barrier, inc=1, device_id={"tp": me + 1}, device_id_type=MESH)

    for q in range(1, n_ep):
        pl.semaphore_signal(barrier, inc=1, device_id={"ep": peer(q)}, device_id_type=MESH)

    experts = n * n_ep
    number = lax.broadcasted_iota(jnp.int32, (experts, tokens), 0)
    base = (lax.rem(number, n) * slots + lax.div(number, n) * cap).astype(f32)
    number = number.astype(f32)
    upper = jnp.where(
        lax.broadcasted_iota(jnp.int32, (tokens, tokens), 0)
        < lax.broadcasted_iota(jnp.int32, (tokens, tokens), 1),
        1.0, 0.0,
    ).astype(bf16)
    used = jnp.zeros((experts, 1), f32)
    for k in range(top):
        hot = jnp.where(number == routes_ref[k : k + 1, :], 1.0, 0.0)
        before = jnp.dot(hot.astype(bf16), upper, preferred_element_type=f32) + used
        meta[me, k : k + 1, :] = jnp.sum((base + before) * hot, axis=0, keepdims=True)
        meta[me, top + k : top + k + 1, :] = routes_ref[top + k : top + k + 1, :]
        used = used + jnp.sum(hot, axis=1, keepdims=True)

    tile_t = 32

    def norm(i):
        at = pl.ds(pl.multiple_of(i * tile_t, tile_t), tile_t)
        held = x_ref[at, :].astype(f32)
        held = held * lax.rsqrt(jnp.mean(held * held, axis=1, keepdims=True) + epsilon)
        held = (held * gain_ref[...]).astype(bf16)
        for c in range(chunks):
            tok[me, c, at, :] = held[:, c * wc : (c + 1) * wc]

    each(tokens // tile_t, norm)

    neighbours = jnp.where(has_left, 1, 0) + jnp.where(has_right, 1, 0)
    pl.semaphore_wait(barrier, n_ep - 1 + neighbours)

    def source(j):
        least = jnp.minimum(me, n - 1 - me)
        k = (j + 1) // 2
        near = jnp.where(j % 2 == 1, me - k, me + k)
        k_far = j - least
        far = jnp.where(me > n - 1 - me, me - k_far, me + k_far)
        return jnp.where(j <= 2 * least, near, far)

    def hop(src, dst, where, send, recv, step):
        return pltpu.make_async_remote_copy(
            src_ref=src.at[where], dst_ref=dst.at[where],
            send_sem=send.at[where], recv_sem=recv.at[where],
            device_id={"tp": me + step}, device_id_type=MESH,
        )

    token_lane = (tok, tok_right, tok_left, tok_recv)
    meta_lane = (meta, meta_right, meta_left, meta_recv)
    pool_lane = (pools, pool_right, pool_left, pool_recv)

    def pass_on(lane, s, where):
        buffer, right, left, recv = lane

        @pl.when((s <= me) & has_right)
        def _():
            hop(buffer, buffer, where, right, recv, 1).start()

        @pl.when((s >= me) & has_left)
        def _():
            hop(buffer, buffer, where, left, recv, -1).start()

    def arrive(lane, where):
        buffer, right, left, recv = lane
        hop(buffer, buffer, where, right, recv, 1).wait_recv()

    def passed(lane, s, where):
        buffer, right, left, recv = lane

        @pl.when((s <= me) & has_right)
        def _():
            hop(buffer, buffer, where, right, recv, 1).wait_send()

        @pl.when((s >= me) & has_left)
        def _():
            hop(buffer, buffer, where, left, recv, -1).wait_send()

    def exchange(src, dst, s, c, p, send, recv):
        return pltpu.make_async_remote_copy(
            src_ref=src.at[s, c, at_slots(p)], dst_ref=dst.at[s, c, at_slots(mine)],
            send_sem=send.at[s, c, p], recv_sem=recv.at[s, c, mine],
            device_id={"ep": p}, device_id_type=MESH,
        )

    def exchanged(dst, s, c, p, send, recv):
        return pltpu.make_async_remote_copy(
            src_ref=dst.at[s, c, at_slots(p)], dst_ref=dst.at[s, c, at_slots(p)],
            send_sem=send.at[s, c, p], recv_sem=recv.at[s, c, p],
            device_id={"ep": p}, device_id_type=MESH,
        )

    def slot_masks(s, use_weight):
        row = lax.broadcasted_iota(jnp.int32, (slots, tokens), 0) + me * slots
        row = row.astype(f32)
        held = meta[s]
        total = jnp.zeros((slots, tokens), f32)
        for k in range(top):
            value = held[top + k : top + k + 1] if use_weight else 1.0
            total = total + jnp.where(row == held[k : k + 1], value, 0.0)
        return total

    tile_h = min(256, d_expert)
    tile_r = min(256, row_count)

    def at_h(i):
        return pl.ds(pl.multiple_of(i * tile_h, tile_h), tile_h)

    def at_r(i):
        return pl.ds(pl.multiple_of(i * tile_r, tile_r), tile_r)

    def dispatch(j):
        s = source(j)

        @pl.when(j > 0)
        def _():
            arrive(meta_lane, (s,))
            pass_on(meta_lane, s, (s,))

        choose = slot_masks(s, False).astype(bf16)

        def chunk(c):
            @pl.when(j > 0)
            def _():
                arrive(token_lane, (s, c))
                pass_on(token_lane, s, (s, c))

            packed[s, c] = jnp.dot(choose, tok[s, c], preferred_element_type=f32).astype(bf16)
            for q in range(1, n_ep):
                exchange(packed, rows, s, c, peer(q), pk_send, pk_recv).start()
            rows[s, c, at_slots(mine)] = packed[s, c, at_slots(mine)]

        each(chunks, chunk)

        @pl.when((s == 0) & has_right)
        def _():
            hop(pools, pools, (me,), pool_right, pool_recv, 1).start()

        @pl.when((s == n - 1) & has_left)
        def _():
            hop(pools, pools, (me,), pool_left, pool_recv, -1).start()

    def expert(s):
        def gather(c):
            for q in range(1, n_ep):
                exchanged(rows, s, c, peer(q), pk_send, pk_recv).wait_recv()

            def inner(i):
                here = rows[s, c]
                gate = jnp.dot(here, wg[at_chunk(c), at_h(i)], preferred_element_type=f32)
                up = jnp.dot(here, wu[at_chunk(c), at_h(i)], preferred_element_type=f32)

                @pl.when(c == 0)
                def _():
                    gates[:, at_h(i)] = gate
                    ups[:, at_h(i)] = up

                @pl.when(c > 0)
                def _():
                    gates[:, at_h(i)] += gate
                    ups[:, at_h(i)] += up

            each(d_expert // tile_h, inner)

        each(chunks, gather)
        gate = gates[...]
        hidden[...] = (gate / (1.0 + jnp.exp(-gate)) * ups[...]).astype(bf16)

        def outer(c):
            rows[s, c] = jnp.dot(
                hidden[...], wd[:, at_chunk(c)], preferred_element_type=f32
            ).astype(bf16)
            for q in range(1, n_ep):
                exchange(rows, back, s, c, peer(q), bk_send, bk_recv).start()
            back[s, c, at_slots(mine)] = rows[s, c, at_slots(mine)]

        each(chunks, outer)

    def combine(s):
        weights = slot_masks(s, True)
        high = weights.astype(bf16)
        low = (weights - high.astype(f32)).astype(bf16)
        dims = (((0,), (0,)), ((), ()))

        def chunk(c):
            for q in range(1, n_ep):
                exchanged(back, s, c, peer(q), bk_send, bk_recv).wait_recv()
            here = back[s, c]
            part[s, c] = (
                lax.dot_general(high, here, dims, preferred_element_type=f32)
                + lax.dot_general(low, here, dims, preferred_element_type=f32)
            ).astype(bf16)

            @pl.when((me == 0) & (s > me))
            def _():
                hop(part, from_left, (s, c), rs_right, rs_right_recv, 1).start()

            @pl.when((me == n - 1) & (s < me))
            def _():
                hop(part, from_right, (s, c), rs_left, rs_left_recv, -1).start()

        each(chunks, chunk)

    def project(s, first):
        def tile(i):
            product = jnp.dot(
                pools[s, at_r(i), :], wo[pl.ds(pl.multiple_of(s * shard, shard), shard), :],
                preferred_element_type=f32,
            )
            acc[at_r(i), :] = product if first else acc[at_r(i), :] + product

        each(row_count // tile_r, tile)

    pass_on(meta_lane, me, (me,))
    each(chunks, lambda c: pass_on(token_lane, me, (me, c)))

    def halo_hop():
        return pltpu.make_async_remote_copy(
            src_ref=pool_ref.at[pl.ds(row_count - halo_depth, halo_depth)], dst_ref=halo,
            send_sem=halo_send.at[0], recv_sem=halo_recv.at[0],
            device_id={"ep": lax.rem(mine + 1, n_ep)}, device_id_type=MESH,
        )

    @pl.when(mine < n_ep - 1)
    def _():
        halo_hop().start()

    def widen(i):
        at = pl.ds(pl.multiple_of(i * tile_r + halo_depth, 16), tile_r)
        extended[at, :] = pool_ref[at_r(i), :].astype(f32)

    each(row_count // tile_r, widen)

    @pl.when(mine == 0)
    def _():
        extended[0:halo_depth, :] = jnp.zeros((halo_depth, shard), f32)

    @pl.when(mine > 0)
    def _():
        halo_hop().wait_recv()
        extended[0:halo_depth, :] = halo[...].astype(f32)

    tile_p = min(128, row_count)

    def pooling(i):
        start = pl.multiple_of(i * tile_p, tile_p)
        for g in range(groups_local):
            group = me * groups_local + g
            turn = lax.rem(group, 4)
            lanes = slice(g * group_dim, (g + 1) * group_dim)
            held = extended[pl.ds(start, tile_p + halo_depth), lanes]
            two = held[1:] + held[:-1]
            four = two[2:] + two[:-2]
            eight = four[4:] + four[:-4]
            sixteen = eight[8:] + eight[:-8]
            summed = jnp.where(
                turn == 0, two[15:],
                jnp.where(turn == 1, four[13:], jnp.where(turn == 2, eight[9:], sixteen[1:])),
            )
            window = jnp.where(
                turn == 0, 2, jnp.where(turn == 1, 4, jnp.where(turn == 2, 8, 16))
            )
            place = lax.broadcasted_iota(jnp.int32, (tile_p, group_dim), 0)
            place = place + (mine * row_count + start + 1)
            counted = jnp.minimum(place, window).astype(f32)
            pooled = (summed / counted - held[halo_depth:]).astype(bf16)
            mapped = jnp.dot(pooled, map_ref[group], preferred_element_type=f32)
            pools[me, pl.ds(start, tile_p), lanes] = (mapped * scale_ref[group]).astype(bf16)

    each(row_count // tile_p, pooling)
    loads[3].wait()
    project(me, True)

    def step(j):
        @pl.when(j < n)
        def _():
            dispatch(j)

        @pl.when(j == 1)
        def _():
            for load in loads[:3]:
                load.wait()

        @pl.when((j >= 1) & (j <= n))
        def _():
            expert(source(j - 1))

        @pl.when(j >= 2)
        def _():
            combine(source(j - 2))

    each(n + 2, step)

    def add_on(buffer, d, send, recv, to):
        def chunk(c):
            hop(part, buffer, (d, c), send, recv, to).wait_recv()
            buffer[d, c] = (buffer[d, c].astype(f32) + part[d, c].astype(f32)).astype(bf16)
            hop(buffer, buffer, (d, c), send, recv, to).start()

        each(chunks, chunk)

    def tail(i):
        s = source(i + 1)
        arrive(pool_lane, (s,))
        pass_on(pool_lane, s, (s,))
        project(s, False)
        right, left = i + 1, n - 2 - i

        @pl.when((me > 0) & (me < right))
        def _():
            add_on(from_left, right, rs_right, rs_right_recv, 1)

        @pl.when((me < n - 1) & (me > left))
        def _():
            add_on(from_right, left, rs_left, rs_left_recv, -1)

    each(n - 1, tail)
    pool_out[...] = acc[...].astype(bf16)

    for c in range(chunks):
        columns = slice(c * wc, (c + 1) * wc)

        @pl.when(has_left)
        def _():
            hop(part, from_left, (me, c), rs_right, rs_right_recv, 1).wait_recv()

        @pl.when(has_right)
        def _():
            hop(part, from_right, (me, c), rs_left, rs_left_recv, -1).wait_recv()

        @pl.when(has_left & has_right)
        def _():
            expert_out[:, columns] = (
                part[me, c].astype(f32)
                + from_left[me, c].astype(f32)
                + from_right[me, c].astype(f32)
            ).astype(bf16)

        @pl.when(has_left & jnp.logical_not(has_right))
        def _():
            expert_out[:, columns] = (
                part[me, c].astype(f32) + from_left[me, c].astype(f32)
            ).astype(bf16)

        @pl.when(has_right & jnp.logical_not(has_left))
        def _():
            expert_out[:, columns] = (
                part[me, c].astype(f32) + from_right[me, c].astype(f32)
            ).astype(bf16)

    @pl.when(mine < n_ep - 1)
    def _():
        halo_hop().wait_send()

    def drain(s):
        passed(meta_lane, s, (s,))
        passed(pool_lane, s, (s,))

        def chunk(c):
            passed(token_lane, s, (s, c))
            for q in range(1, n_ep):
                exchange(packed, rows, s, c, peer(q), pk_send, pk_recv).wait_send()
                exchange(rows, back, s, c, peer(q), bk_send, bk_recv).wait_send()

            @pl.when(me < s)
            def _():
                hop(part, from_left, (s, c), rs_right, rs_right_recv, 1).wait_send()

            @pl.when(me > s)
            def _():
                hop(part, from_right, (s, c), rs_left, rs_left_recv, -1).wait_send()

        each(chunks, chunk)

    each(n, drain)


def on_device(
    pool_input, pool_map, pool_scale, out_weight, expert_input, norm_gain,
    routes, route_weight, gate_weight, up_weight, down_weight,
):
    n_ep, n = lax.axis_size("ep"), lax.axis_size("tp")
    tokens, width = expert_input.shape
    top = routes.shape[1]
    cap = max(2 * tokens * top // (n_ep * n), 16)
    slots = n_ep * cap
    chunks = max(1, min(4, 64 // (n_ep * n)))
    wc = width // chunks
    row_count, shard = pool_input.shape
    groups, group_dim = pool_map.shape[:2]
    meta = jnp.concatenate([routes.astype(f32), route_weight.astype(f32)], axis=1).T
    meta = jnp.pad(meta, ((0, -meta.shape[0] % 8), (0, 0)))
    d_expert = gate_weight.shape[2]
    dma = pltpu.SemaphoreType.DMA
    vmem = pl.BlockSpec(memory_space=pltpu.VMEM)
    hbm = pl.BlockSpec(memory_space=pl.ANY)
    one, line, grid, pair = dma((1,)), dma((n,)), dma((n, chunks)), dma((n, chunks, n_ep))
    by_slot = pltpu.VMEM((n, chunks, slots, wc), bf16)
    by_token = pltpu.VMEM((n, chunks, tokens, wc), bf16)
    out_columns = out_weight.shape[1]
    return pl.pallas_call(
        functools.partial(kernel, n, n_ep, cap, top, chunks),
        out_shape=(
            jax.ShapeDtypeStruct((row_count, out_columns), bf16),
            jax.ShapeDtypeStruct((tokens, width), bf16),
        ),
        in_specs=[vmem] * 6 + [hbm] * 4,
        out_specs=(vmem, vmem),
        scratch_shapes=[
            pltpu.VMEM((width, d_expert), bf16),
            pltpu.VMEM((width, d_expert), bf16),
            pltpu.VMEM((d_expert, width), bf16),
            pltpu.VMEM(out_weight.shape, bf16),
            by_token,
            pltpu.VMEM((n,) + meta.shape, f32),
            pltpu.VMEM((n, row_count, shard), bf16),
            by_slot, by_slot, by_slot,
            pltpu.VMEM((slots, d_expert), f32),
            pltpu.VMEM((slots, d_expert), f32),
            pltpu.VMEM((slots, d_expert), bf16),
            by_token, by_token, by_token,
            pltpu.VMEM((row_count, out_columns), f32),
            pltpu.VMEM((halo_depth, shard), bf16),
            pltpu.VMEM((row_count + halo_depth, shard), f32),
            dma((4,)), one, one,
            grid, grid, grid, line, line, line, line, line, line,
            pair, pair, pair, pair,
            grid, grid, grid, grid,
        ],
        compiler_params=pltpu.CompilerParams(
            collective_id=0, has_side_effects=True, vmem_limit_bytes=62 * 1024 * 1024
        ),
    )(
        expert_input, norm_gain.reshape(1, width), meta, pool_input, pool_map,
        pool_scale.reshape(groups, 1, group_dim), gate_weight, up_weight, down_weight, out_weight,
    )


def solution(mesh):
    return jax.shard_map(
        on_device,
        mesh=mesh,
        in_specs=(
            P(("grp", "ep"), "tp"),
            P(),
            P(),
            P(None, "tp"),
            P(("grp", "ep", "tp"), None),
            P(),
            P(("grp", "ep", "tp"), None),
            P(("grp", "ep", "tp"), None),
            P(("ep", "tp"), None, None),
            P(("ep", "tp"), None, None),
            P(("ep", "tp"), None, None),
        ),
        out_specs=(P(("grp", "ep"), "tp"), P(("grp", "ep", "tp"), None)),
        check_vma=False,
    )
```

```python
import functools

import jax
import jax.numpy as jnp
from jax import lax
from jax.experimental import pallas as pl
from jax.experimental.pallas import tpu as pltpu
from jax.sharding import PartitionSpec as P

epsilon = 1e-06
halo_depth = 16
MESH = pl.DeviceIdType.MESH
bf16 = jnp.bfloat16
f32 = jnp.float32


def kernel(
    n, n_ep, cap, top, chunks,
    x_ref, gain_ref, routes_ref, pool_ref, map_ref, scale_ref, gate_hbm, up_hbm, down_hbm, out_w_hbm,
    pool_out, expert_out,
    wg, wu, wd, wo, tok, meta, pools, packed, rows, back, gates, ups, hidden,
    part, from_left, from_right, acc, halo, extended,
    w_sem, halo_send, halo_recv, tok_recv, tok_right, tok_left, meta_recv, meta_right, meta_left,
    pool_recv, pool_right, pool_left, pk_send, pk_recv, bk_send, bk_recv,
    rs_right, rs_right_recv, rs_left, rs_left_recv,
):
    me = lax.axis_index("tp")
    mine = lax.axis_index("ep")
    tokens, width = x_ref.shape
    slots = n_ep * cap
    d_expert = wg.shape[1]
    row_count, shard = pool_ref.shape
    group_dim = map_ref.shape[1]
    groups_local = shard // group_dim
    wc = width // chunks
    has_left, has_right = me > 0, me < n - 1

    def peer(q):
        return lax.rem(mine + q, n_ep)

    def at_slots(p):
        return pl.ds(pl.multiple_of(p * cap, cap), cap)

    def at_chunk(c):
        return pl.ds(pl.multiple_of(c * wc, wc), wc)

    def each(count, body):
        def run(i, _):
            body(i)
            return 0

        lax.fori_loop(0, count, run, 0)

    loads = [
        pltpu.make_async_copy(src, dst, w_sem.at[i])
        for i, (src, dst) in enumerate(
            ((gate_hbm.at[0], wg), (up_hbm.at[0], wu), (down_hbm.at[0], wd), (out_w_hbm, wo))
        )
    ]
    for load in loads:
        load.start()

    barrier = pltpu.get_barrier_semaphore()

    @pl.when(has_left)
    def _():
        pl.semaphore_signal(barrier, inc=1, device_id={"tp": me - 1}, device_id_type=MESH)

    @pl.when(has_right)
    def _():
        pl.semaphore_signal(barrier, inc=1, device_id={"tp": me + 1}, device_id_type=MESH)

    for q in range(1, n_ep):
        pl.semaphore_signal(barrier, inc=1, device_id={"ep": peer(q)}, device_id_type=MESH)

    experts = n * n_ep
    number = lax.broadcasted_iota(jnp.int32, (experts, tokens), 0)
    base = (lax.rem(number, n) * slots + lax.div(number, n) * cap).astype(f32)
    number = number.astype(f32)
    upper = jnp.where(
        lax.broadcasted_iota(jnp.int32, (tokens, tokens), 0)
        < lax.broadcasted_iota(jnp.int32, (tokens, tokens), 1),
        1.0, 0.0,
    ).astype(bf16)
    used = jnp.zeros((experts, 1), f32)
    for k in range(top):
        hot = jnp.where(number == routes_ref[k : k + 1, :], 1.0, 0.0)
        before = jnp.dot(hot.astype(bf16), upper, preferred_element_type=f32) + used
        meta[me, k : k + 1, :] = jnp.sum((base + before) * hot, axis=0, keepdims=True)
        meta[me, top + k : top + k + 1, :] = routes_ref[top + k : top + k + 1, :]
        used = used + jnp.sum(hot, axis=1, keepdims=True)

    tile_t = 32

    def norm(i):
        at = pl.ds(pl.multiple_of(i * tile_t, tile_t), tile_t)
        held = x_ref[at, :].astype(f32)
        held = held * lax.rsqrt(jnp.mean(held * held, axis=1, keepdims=True) + epsilon)
        held = (held * gain_ref[...]).astype(bf16)
        for c in range(chunks):
            tok[me, c, at, :] = held[:, c * wc : (c + 1) * wc]

    each(tokens // tile_t, norm)

    neighbours = jnp.where(has_left, 1, 0) + jnp.where(has_right, 1, 0)
    pl.semaphore_wait(barrier, n_ep - 1 + neighbours)

    def source(j):
        least = jnp.minimum(me, n - 1 - me)
        k = (j + 1) // 2
        near = jnp.where(j % 2 == 1, me - k, me + k)
        k_far = j - least
        far = jnp.where(me > n - 1 - me, me - k_far, me + k_far)
        return jnp.where(j <= 2 * least, near, far)

    def hop(src, dst, where, send, recv, step):
        return pltpu.make_async_remote_copy(
            src_ref=src.at[where], dst_ref=dst.at[where],
            send_sem=send.at[where], recv_sem=recv.at[where],
            device_id={"tp": me + step}, device_id_type=MESH,
        )

    token_lane = (tok, tok_right, tok_left, tok_recv)
    meta_lane = (meta, meta_right, meta_left, meta_recv)
    pool_lane = (pools, pool_right, pool_left, pool_recv)

    def pass_on(lane, s, where):
        buffer, right, left, recv = lane

        @pl.when((s <= me) & has_right)
        def _():
            hop(buffer, buffer, where, right, recv, 1).start()

        @pl.when((s >= me) & has_left)
        def _():
            hop(buffer, buffer, where, left, recv, -1).start()

    def arrive(lane, where):
        buffer, right, left, recv = lane
        hop(buffer, buffer, where, right, recv, 1).wait_recv()

    def passed(lane, s, where):
        buffer, right, left, recv = lane

        @pl.when((s <= me) & has_right)
        def _():
            hop(buffer, buffer, where, right, recv, 1).wait_send()

        @pl.when((s >= me) & has_left)
        def _():
            hop(buffer, buffer, where, left, recv, -1).wait_send()

    def exchange(src, dst, s, c, p, send, recv):
        return pltpu.make_async_remote_copy(
            src_ref=src.at[s, c, at_slots(p)], dst_ref=dst.at[s, c, at_slots(mine)],
            send_sem=send.at[s, c, p], recv_sem=recv.at[s, c, mine],
            device_id={"ep": p}, device_id_type=MESH,
        )

    def exchanged(dst, s, c, p, send, recv):
        return pltpu.make_async_remote_copy(
            src_ref=dst.at[s, c, at_slots(p)], dst_ref=dst.at[s, c, at_slots(p)],
            send_sem=send.at[s, c, p], recv_sem=recv.at[s, c, p],
            device_id={"ep": p}, device_id_type=MESH,
        )

    def slot_masks(s, use_weight):
        row = lax.broadcasted_iota(jnp.int32, (slots, tokens), 0) + me * slots
        row = row.astype(f32)
        held = meta[s]
        total = jnp.zeros((slots, tokens), f32)
        for k in range(top):
            value = held[top + k : top + k + 1] if use_weight else 1.0
            total = total + jnp.where(row == held[k : k + 1], value, 0.0)
        return total

    tile_h = min(256, d_expert)
    tile_r = min(256, row_count)

    def at_h(i):
        return pl.ds(pl.multiple_of(i * tile_h, tile_h), tile_h)

    def at_r(i):
        return pl.ds(pl.multiple_of(i * tile_r, tile_r), tile_r)

    def dispatch(j):
        s = source(j)

        @pl.when(j > 0)
        def _():
            arrive(meta_lane, (s,))
            pass_on(meta_lane, s, (s,))

        choose = slot_masks(s, False).astype(bf16)

        def chunk(c):
            @pl.when(j > 0)
            def _():
                arrive(token_lane, (s, c))
                pass_on(token_lane, s, (s, c))

            packed[s, c] = jnp.dot(choose, tok[s, c], preferred_element_type=f32).astype(bf16)
            for q in range(1, n_ep):
                exchange(packed, rows, s, c, peer(q), pk_send, pk_recv).start()
            rows[s, c, at_slots(mine)] = packed[s, c, at_slots(mine)]

        each(chunks, chunk)

        @pl.when((s == 0) & has_right)
        def _():
            hop(pools, pools, (me,), pool_right, pool_recv, 1).start()

        @pl.when((s == n - 1) & has_left)
        def _():
            hop(pools, pools, (me,), pool_left, pool_recv, -1).start()

    def expert(s):
        def gather(c):
            for q in range(1, n_ep):
                exchanged(rows, s, c, peer(q), pk_send, pk_recv).wait_recv()

            def inner(i):
                here = rows[s, c]
                gate = jnp.dot(here, wg[at_chunk(c), at_h(i)], preferred_element_type=f32)
                up = jnp.dot(here, wu[at_chunk(c), at_h(i)], preferred_element_type=f32)

                @pl.when(c == 0)
                def _():
                    gates[:, at_h(i)] = gate
                    ups[:, at_h(i)] = up

                @pl.when(c > 0)
                def _():
                    gates[:, at_h(i)] += gate
                    ups[:, at_h(i)] += up

            each(d_expert // tile_h, inner)

        each(chunks, gather)
        gate = gates[...]
        hidden[...] = (gate / (1.0 + jnp.exp(-gate)) * ups[...]).astype(bf16)

        def outer(c):
            rows[s, c] = jnp.dot(
                hidden[...], wd[:, at_chunk(c)], preferred_element_type=f32
            ).astype(bf16)
            for q in range(1, n_ep):
                exchange(rows, back, s, c, peer(q), bk_send, bk_recv).start()
            back[s, c, at_slots(mine)] = rows[s, c, at_slots(mine)]

        each(chunks, outer)

    def combine(s):
        weights = slot_masks(s, True)
        high = weights.astype(bf16)
        low = (weights - high.astype(f32)).astype(bf16)
        dims = (((0,), (0,)), ((), ()))

        def chunk(c):
            for q in range(1, n_ep):
                exchanged(back, s, c, peer(q), bk_send, bk_recv).wait_recv()
            here = back[s, c]
            part[s, c] = (
                lax.dot_general(high, here, dims, preferred_element_type=f32)
                + lax.dot_general(low, here, dims, preferred_element_type=f32)
            ).astype(bf16)

            @pl.when((me == 0) & (s > me))
            def _():
                hop(part, from_left, (s, c), rs_right, rs_right_recv, 1).start()

            @pl.when((me == n - 1) & (s < me))
            def _():
                hop(part, from_right, (s, c), rs_left, rs_left_recv, -1).start()

        each(chunks, chunk)

    def project(s, first):
        def tile(i):
            product = jnp.dot(
                pools[s, at_r(i), :], wo[pl.ds(pl.multiple_of(s * shard, shard), shard), :],
                preferred_element_type=f32,
            )
            acc[at_r(i), :] = product if first else acc[at_r(i), :] + product

        each(row_count // tile_r, tile)

    pass_on(meta_lane, me, (me,))
    each(chunks, lambda c: pass_on(token_lane, me, (me, c)))

    def halo_hop():
        return pltpu.make_async_remote_copy(
            src_ref=pool_ref.at[pl.ds(row_count - halo_depth, halo_depth)], dst_ref=halo,
            send_sem=halo_send.at[0], recv_sem=halo_recv.at[0],
            device_id={"ep": lax.rem(mine + 1, n_ep)}, device_id_type=MESH,
        )

    @pl.when(mine < n_ep - 1)
    def _():
        halo_hop().start()

    def widen(i):
        at = pl.ds(pl.multiple_of(i * tile_r + halo_depth, 16), tile_r)
        extended[at, :] = pool_ref[at_r(i), :].astype(f32)

    each(row_count // tile_r, widen)

    @pl.when(mine == 0)
    def _():
        extended[0:halo_depth, :] = jnp.zeros((halo_depth, shard), f32)

    @pl.when(mine > 0)
    def _():
        halo_hop().wait_recv()
        extended[0:halo_depth, :] = halo[...].astype(f32)

    tile_p = min(128, row_count)

    def pooling(i):
        start = pl.multiple_of(i * tile_p, tile_p)
        for g in range(groups_local):
            group = me * groups_local + g
            turn = lax.rem(group, 4)
            lanes = slice(g * group_dim, (g + 1) * group_dim)
            held = extended[pl.ds(start, tile_p + halo_depth), lanes]
            two = held[1:] + held[:-1]
            four = two[2:] + two[:-2]
            eight = four[4:] + four[:-4]
            sixteen = eight[8:] + eight[:-8]
            summed = jnp.where(
                turn == 0, two[15:],
                jnp.where(turn == 1, four[13:], jnp.where(turn == 2, eight[9:], sixteen[1:])),
            )
            window = jnp.where(
                turn == 0, 2, jnp.where(turn == 1, 4, jnp.where(turn == 2, 8, 16))
            )
            place = lax.broadcasted_iota(jnp.int32, (tile_p, group_dim), 0)
            place = place + (mine * row_count + start + 1)
            counted = jnp.minimum(place, window).astype(f32)
            pooled = (summed / counted - held[halo_depth:]).astype(bf16)
            mapped = jnp.dot(pooled, map_ref[group], preferred_element_type=f32)
            pools[me, pl.ds(start, tile_p), lanes] = (mapped * scale_ref[group]).astype(bf16)

    each(row_count // tile_p, pooling)
    loads[3].wait()
    project(me, True)

    behind = jnp.where(has_left & has_right, 1, 0)

    def take_pool(j):
        s = source(j)
        arrive(pool_lane, (s,))
        pass_on(pool_lane, s, (s,))
        project(s, False)

    def step(j):
        at_expert = j - behind
        at_combine = at_expert - 1

        @pl.when(j < n)
        def _():
            dispatch(j)

        @pl.when(at_expert == 0)
        def _():
            for load in loads[:3]:
                load.wait()

        @pl.when((at_combine >= 0) & (at_combine < n))
        def _():
            combine(source(at_combine))

        @pl.when((at_expert >= 0) & (at_expert < n))
        def _():
            expert(source(at_expert))

    each(n + 2, step)

    def add_on(buffer, d, c, send, recv, to):
        hop(part, buffer, (d, c), send, recv, to).wait_recv()
        buffer[d, c] = (buffer[d, c].astype(f32) + part[d, c].astype(f32)).astype(bf16)
        hop(buffer, buffer, (d, c), send, recv, to).start()

    take_pool(1)

    def tail(i):
        right, left = i + 1, n - 2 - i

        def chunk(c):
            @pl.when((me > 0) & (me < right))
            def _():
                add_on(from_left, right, c, rs_right, rs_right_recv, 1)

            @pl.when((me < n - 1) & (me > left))
            def _():
                add_on(from_right, left, c, rs_left, rs_left_recv, -1)

        each(chunks, chunk)

        @pl.when(i + 2 < n)
        def _():
            take_pool(i + 2)

    each(n - 1, tail)
    pool_out[...] = acc[...].astype(bf16)

    for c in range(chunks):
        columns = slice(c * wc, (c + 1) * wc)

        @pl.when(has_left)
        def _():
            hop(part, from_left, (me, c), rs_right, rs_right_recv, 1).wait_recv()

        @pl.when(has_right)
        def _():
            hop(part, from_right, (me, c), rs_left, rs_left_recv, -1).wait_recv()

        @pl.when(has_left & has_right)
        def _():
            expert_out[:, columns] = (
                part[me, c].astype(f32)
                + from_left[me, c].astype(f32)
                + from_right[me, c].astype(f32)
            ).astype(bf16)

        @pl.when(has_left & jnp.logical_not(has_right))
        def _():
            expert_out[:, columns] = (
                part[me, c].astype(f32) + from_left[me, c].astype(f32)
            ).astype(bf16)

        @pl.when(has_right & jnp.logical_not(has_left))
        def _():
            expert_out[:, columns] = (
                part[me, c].astype(f32) + from_right[me, c].astype(f32)
            ).astype(bf16)

    @pl.when(mine < n_ep - 1)
    def _():
        halo_hop().wait_send()

    def drain(s):
        passed(meta_lane, s, (s,))
        passed(pool_lane, s, (s,))

        def chunk(c):
            passed(token_lane, s, (s, c))
            for q in range(1, n_ep):
                exchange(packed, rows, s, c, peer(q), pk_send, pk_recv).wait_send()
                exchange(rows, back, s, c, peer(q), bk_send, bk_recv).wait_send()

            @pl.when(me < s)
            def _():
                hop(part, from_left, (s, c), rs_right, rs_right_recv, 1).wait_send()

            @pl.when(me > s)
            def _():
                hop(part, from_right, (s, c), rs_left, rs_left_recv, -1).wait_send()

        each(chunks, chunk)

    each(n, drain)


def on_device(
    pool_input, pool_map, pool_scale, out_weight, expert_input, norm_gain,
    routes, route_weight, gate_weight, up_weight, down_weight,
):
    n_ep, n = lax.axis_size("ep"), lax.axis_size("tp")
    tokens, width = expert_input.shape
    top = routes.shape[1]
    cap = max(2 * tokens * top // (n_ep * n), 16)
    slots = n_ep * cap
    chunks = max(1, min(4, 64 // (n_ep * n)))
    wc = width // chunks
    row_count, shard = pool_input.shape
    groups, group_dim = pool_map.shape[:2]
    meta = jnp.concatenate([routes.astype(f32), route_weight.astype(f32)], axis=1).T
    meta = jnp.pad(meta, ((0, -meta.shape[0] % 8), (0, 0)))
    d_expert = gate_weight.shape[2]
    dma = pltpu.SemaphoreType.DMA
    vmem = pl.BlockSpec(memory_space=pltpu.VMEM)
    hbm = pl.BlockSpec(memory_space=pl.ANY)
    one, line, grid, pair = dma((1,)), dma((n,)), dma((n, chunks)), dma((n, chunks, n_ep))
    by_slot = pltpu.VMEM((n, chunks, slots, wc), bf16)
    by_token = pltpu.VMEM((n, chunks, tokens, wc), bf16)
    out_columns = out_weight.shape[1]
    return pl.pallas_call(
        functools.partial(kernel, n, n_ep, cap, top, chunks),
        out_shape=(
            jax.ShapeDtypeStruct((row_count, out_columns), bf16),
            jax.ShapeDtypeStruct((tokens, width), bf16),
        ),
        in_specs=[vmem] * 6 + [hbm] * 4,
        out_specs=(vmem, vmem),
        scratch_shapes=[
            pltpu.VMEM((width, d_expert), bf16),
            pltpu.VMEM((width, d_expert), bf16),
            pltpu.VMEM((d_expert, width), bf16),
            pltpu.VMEM(out_weight.shape, bf16),
            by_token,
            pltpu.VMEM((n,) + meta.shape, f32),
            pltpu.VMEM((n, row_count, shard), bf16),
            by_slot, by_slot, by_slot,
            pltpu.VMEM((slots, d_expert), f32),
            pltpu.VMEM((slots, d_expert), f32),
            pltpu.VMEM((slots, d_expert), bf16),
            by_token, by_token, by_token,
            pltpu.VMEM((row_count, out_columns), f32),
            pltpu.VMEM((halo_depth, shard), bf16),
            pltpu.VMEM((row_count + halo_depth, shard), f32),
            dma((4,)), one, one,
            grid, grid, grid, line, line, line, line, line, line,
            pair, pair, pair, pair,
            grid, grid, grid, grid,
        ],
        compiler_params=pltpu.CompilerParams(
            collective_id=0, has_side_effects=True, vmem_limit_bytes=62 * 1024 * 1024
        ),
    )(
        expert_input, norm_gain.reshape(1, width), meta, pool_input, pool_map,
        pool_scale.reshape(groups, 1, group_dim), gate_weight, up_weight, down_weight, out_weight,
    )


def solution(mesh):
    return jax.shard_map(
        on_device,
        mesh=mesh,
        in_specs=(
            P(("grp", "ep"), "tp"),
            P(),
            P(),
            P(None, "tp"),
            P(("grp", "ep", "tp"), None),
            P(),
            P(("grp", "ep", "tp"), None),
            P(("grp", "ep", "tp"), None),
            P(("ep", "tp"), None, None),
            P(("ep", "tp"), None, None),
            P(("ep", "tp"), None, None),
        ),
        out_specs=(P(("grp", "ep"), "tp"), P(("grp", "ep", "tp"), None)),
        check_vma=False,
    )
```
